32 devices in a mesh: sp: 16 (over z, y, x), tp: 2 (over core).
Axes of the slice: x: 2, y: 2, z: 4, core: 2. Of those that a mesh axis runs over, the one named last changes fastest.
Arguments:
- residual: bfloat16 [6144, 2048], P('sp'), may hold values from -6 to 6
- queries: bfloat16 [6144, 2048], P('sp', 'tp'), may hold values from -48 to 48
- keys: bfloat16 [6144, 2048], P('sp', 'tp'), may hold values from -48 to 48
- values: bfloat16 [6144, 2048], P('sp', 'tp'), may hold values from -6 to 6
- gate_cache: float32 [6144, 32], P('sp', 'tp'), may hold values from -1544 to 0, as said below
- doc_ids: int32 [6144], P('sp'), may hold values from 0 to 7, never falling along the last dimension, each value on 1 to 1536 neighbouring positions
- out_weight: bfloat16 [2048, 2048], P('tp'), may hold values from -1 to 1
- mix_gain: float32 [2048], replicated, may hold values from 0.1 to 1.9
- gate_weight: bfloat16 [2048, 5120], P('sp', 'tp'), may hold values from -0.125 to 0.125
- up_weight: bfloat16 [2048, 5120], P('sp', 'tp'), may hold values from -0.125 to 0.125
- down_weight: bfloat16 [5120, 2048], P('tp', 'sp'), may hold values from -0.15625 to 0.15625
Outputs:
- layer_out: bfloat16 [6144, 2048], P(('sp', 'tp'))
The draws below stay inside these ranges and needn't reach their ends.
Inputs may be any that keep to these rules, and one draw needn't show every extreme that they name: `doc_ids`: positions of one document are consecutive; each document has 1 to 1536 positions, and one has exactly that many. `gate_cache`: no column rises from one position to the next.
All inputs are finite; a program needn't handle non-finite values.
Results may differ from the reference program's by a relative error of at most 0.018.
Values may be sent and summed in bfloat16 or wider, within the bound.
A program may use at most 128 MiB of HBM per device.

```python
import math
import jax
import jax.numpy as jnp
import numpy as np
from jax import lax

D = 2048
HEAD_COUNT = 32
HEAD_DIM = 64
FF = 5120
REACH = 4
TOK_DEV = 384
TOKEN_COUNT = 6144
DOCS = 8
N_TP = 2


def drawn(key):
    base_key = jax.random.fold_in(key, 11)
    key_q, key_k = jax.random.split(base_key, 2)
    col_count = HEAD_COUNT * HEAD_DIM
    queries = jax.random.normal(key_q, (TOKEN_COUNT, col_count), jnp.float32)
    keys = jax.random.normal(key_k, (TOKEN_COUNT, col_count), jnp.float32)
    return (jnp.clip(queries, -48.0, 48.0), jnp.clip(keys, -48.0, 48.0))


def draw_queries(key, part):
    return drawn(key)[0].astype(jnp.bfloat16)


def draw_keys(key, part):
    return drawn(key)[1].astype(jnp.bfloat16)


def draw_gate_cache(key, part):
    base_key = jax.random.fold_in(key, 23)
    key_h, key_r, key_s, key_b, key_u, key_position, key_document = jax.random.split(base_key, 7)
    head_order = jax.random.permutation(key_h, HEAD_COUNT)
    slow_heads = head_order < HEAD_COUNT // 2
    fast_rate = jnp.exp(jax.random.uniform(key_r, (HEAD_COUNT,), jnp.float32, math.log(1.0 / 100.0), math.log(1.0 / 30.0)))
    slow_rate = jax.random.uniform(key_s, (HEAD_COUNT,), jnp.float32, 0.5, 2.0) / TOKEN_COUNT
    head_rate = jnp.where(slow_heads, slow_rate, fast_rate)
    blocks = TOKEN_COUNT // TOK_DEV
    factor = jnp.exp(jax.random.uniform(key_b, (blocks,), jnp.float32, math.log(0.4), math.log(2.5)))
    factor_rows = jnp.repeat(factor, TOK_DEV)
    wobble = jax.random.uniform(key_u, (TOKEN_COUNT, HEAD_COUNT), jnp.float32, 0.2, 1.8)
    logarithm_gate = -head_rate[None, :] * factor_rows[:, None] * wobble
    spike_start = jax.random.randint(key_position, (8,), 0, TOKEN_COUNT)
    spike_length = jnp.log(jax.random.uniform(key_document, (8, HEAD_COUNT), jnp.float32, 0.5, 0.8))
    logarithm_gate = logarithm_gate.at[spike_start].add(spike_length)
    return jnp.cumsum(logarithm_gate, axis=0)


def block_scale(stream_key, shape, cuts, least, largest):
    def one(position, parts):
        heights = jax.random.uniform(jax.random.fold_in(jax.random.fold_in(stream_key, 6), position), (parts,), jnp.float32, least / len(cuts), largest / len(cuts))
        return jnp.repeat(jnp.exp(heights), shape[position] // parts).reshape((-1,) + (1,) * (len(shape) - position - 1))

    loudness = one(*cuts[0])
    for cut in cuts[1:]:
        loudness = loudness * one(*cut)
    return loudness


def length_profile(amount, total, limit, slope):
    portions = [(1 << 20) // math.isqrt(rank ** slope) + 1 for rank in range(2, amount + 1)]
    surplus, given = total - limit - (amount - 1), [1] * (amount - 1)
    while surplus > 0:
        candidates = [i for i in range(amount - 1) if given[i] < limit]
        whole, remaining = sum([portions[i] for i in candidates]), surplus
        for i in candidates:
            addition = min(limit - given[i], max(1, remaining * portions[i] // whole), surplus)
            given[i] = given[i] + addition
            surplus = surplus - addition
    return np.array([limit] + given)


def ragged_sizes(rng, count, total, most, slope):
    if count == 2:
        one = jax.random.randint(rng, (), max(1, total - most), min(most, total - 1) + 1)
        return jnp.stack([one, total - one])
    tallies = jnp.asarray(length_profile(count, total, most, slope), jnp.int32)
    twos = (count - 1) // 2
    source_of, taker = tallies[1:1 + 2 * twos:2], tallies[2:2 + 2 * twos:2]
    margin = jnp.minimum(source_of - 1, most - taker)
    shifted = jax.random.randint(jax.random.fold_in(rng, 1), (twos,), 0, 1 << 20) % (margin + 1)
    tallies = tallies.at[1:1 + 2 * twos:2].set(source_of - shifted).at[2:2 + 2 * twos:2].set(taker + shifted)
    return tallies[jax.random.permutation(jax.random.fold_in(rng, 2), count)]


def noise(rng, dims, scale, reach, pieces=(), held_as=jnp.bfloat16):
    level = block_scale(rng, dims, pieces, -0.22, 0.18) if pieces else 1.0
    drawn = jax.random.normal(rng, dims, jnp.float32) * scale * level
    return jnp.minimum(jnp.maximum(drawn, -reach), reach).astype(held_as)


def setup_inputs(seed: int = 0) -> dict:
    streams_of = jax.random.split(jax.random.key(seed), 12)
    return {
        "residual": noise(streams_of[0], (TOKEN_COUNT, D), 1.0, 6.0, ((0, 16),)),
        "queries": draw_queries(jax.random.fold_in(streams_of[11], 71), 0),
        "keys": draw_keys(jax.random.fold_in(streams_of[11], 71), 0),
        "values": noise(streams_of[3], (TOKEN_COUNT, HEAD_COUNT * HEAD_DIM), 1.0, 6.0, ((0, 16), (1, 2))),
        "gate_cache": draw_gate_cache(jax.random.fold_in(streams_of[11], 71), 0),
        "doc_ids": jnp.searchsorted(jnp.cumsum(ragged_sizes(streams_of[5], DOCS, TOKEN_COUNT, REACH * TOK_DEV, 0)), jnp.arange(TOKEN_COUNT), side="right").astype(jnp.int32),
        "out_weight": noise(streams_of[6], (HEAD_COUNT * HEAD_DIM, D), (HEAD_COUNT * HEAD_DIM // 64) ** -0.5, 1.0, ((0, 2),)),
        "mix_gain": jnp.clip(1.0 + 0.18 * jax.random.normal(streams_of[7], (D,), jnp.float32), 0.1, 1.9),
        "gate_weight": noise(streams_of[8], (D, FF), D ** -0.5, 0.125, ((0, 16), (1, 2))),
        "up_weight": noise(streams_of[9], (D, FF), D ** -0.5, 0.125, ((0, 16), (1, 2))),
        "down_weight": noise(streams_of[10], (FF, D), (FF // 4) ** -0.5, 0.15625, ((0, 2), (1, 16))),
    }


EPSILON = 1e-06
NEGATIVE = -1e+30

def group_sum(activations, weight, groups):
    row_count = activations.shape[0]
    inner_cols = activations.shape[1] // groups
    left_grouped = activations.reshape(row_count, groups, inner_cols).transpose(1, 0, 2)
    right_grouped = weight.reshape(groups, inner_cols, weight.shape[1])

    def add_group(running, operands):
        partial_value = jnp.dot(operands[0], operands[1], preferred_element_type=jnp.float32)
        rounded = lax.optimization_barrier(partial_value.astype(jnp.bfloat16))
        return (running + rounded.astype(jnp.float32), None)
    zeros_init = jnp.zeros((row_count, weight.shape[1]), jnp.float32)
    running, ignored = lax.scan(add_group, zeros_init, (left_grouped, right_grouped))
    return running

def normalize(middle, gain):
    widened = middle.astype(jnp.float32)
    factor = lax.rsqrt(lax.optimization_barrier(jnp.mean(widened * widened, axis=-1, keepdims=True)) + EPSILON)
    return (widened * factor * gain).astype(jnp.bfloat16)

def attend(queries, keys, values, gate_cache, doc_ids):
    tokens = queries.shape[0]
    doc_span = REACH * TOK_DEV
    block_rows = math.gcd(tokens, 512)
    key_count = doc_span + block_rows
    head_shape = (tokens, HEAD_COUNT, HEAD_DIM)
    query_heads = queries.reshape(head_shape)
    pad_rows = ((doc_span, 0), (0, 0), (0, 0))
    key_heads = jnp.pad(keys.reshape(head_shape), pad_rows)
    value_heads = jnp.pad(values.reshape(head_shape), pad_rows)
    cache_pad = jnp.pad(gate_cache, ((doc_span, 0), (0, 0)))
    docs_pad = jnp.pad(doc_ids, (doc_span, 0), constant_values=-1)
    score_scale = HEAD_DIM ** (-0.5)

    def one_block(block_index):
        start_row = (block_index * block_rows).astype(jnp.int32)
        query_block = lax.dynamic_slice_in_dim(query_heads, start_row, block_rows, 0).astype(jnp.float32)
        key_block = lax.dynamic_slice_in_dim(key_heads, start_row, key_count, 0).astype(jnp.float32)
        value_block = lax.dynamic_slice_in_dim(value_heads, start_row, key_count, 0).astype(jnp.float32)
        query_cache = lax.dynamic_slice_in_dim(gate_cache, start_row, block_rows, 0)
        key_cache = lax.dynamic_slice_in_dim(cache_pad, start_row, key_count, 0)
        query_docs = lax.dynamic_slice_in_dim(doc_ids, start_row, block_rows, 0)
        key_docs = lax.dynamic_slice_in_dim(docs_pad, start_row, key_count, 0)
        query_pos = start_row + jnp.arange(block_rows, dtype=jnp.int32)
        key_pos = start_row - doc_span + jnp.arange(key_count, dtype=jnp.int32)
        visible = (key_pos[None, :] <= query_pos[:, None]) & (key_pos[None, :] >= 0) & (key_docs[None, :] == query_docs[:, None])
        scores = jnp.einsum('qhd,khd->hqk', query_block, key_block) * score_scale
        scores = scores + query_cache.T[:, :, None] - key_cache.T[:, None, :]
        scores = jnp.where(visible[None], scores, NEGATIVE)
        row_max = lax.optimization_barrier(jnp.max(scores, axis=-1, keepdims=True))
        exp_scores = jnp.exp(scores - row_max)
        weights = (exp_scores / lax.optimization_barrier(jnp.sum(exp_scores, axis=-1, keepdims=True))).astype(jnp.bfloat16)
        weights = lax.optimization_barrier(weights)
        mixed_out = jnp.einsum('hqk,khd->qhd', weights.astype(jnp.float32), value_block)
        return mixed_out.astype(jnp.bfloat16)
    blocks = lax.map(one_block, jnp.arange(tokens // block_rows, dtype=jnp.int32))
    return blocks.reshape(tokens, HEAD_COUNT * HEAD_DIM)

def reference(residual, queries, keys, values, gate_cache, doc_ids, out_weight, mix_gain, gate_weight, up_weight, down_weight):
    attended = attend(queries, keys, values, gate_cache, doc_ids)
    projected = group_sum(attended, out_weight, N_TP)
    middle = (residual.astype(jnp.float32) + projected).astype(jnp.bfloat16)
    normed = normalize(middle, mix_gain)
    gate_proj = jnp.dot(normed, gate_weight, preferred_element_type=jnp.float32)
    up_proj = jnp.dot(normed, up_weight, preferred_element_type=jnp.float32)
    hidden = (jax.nn.silu(gate_proj) * up_proj).astype(jnp.bfloat16)
    lowered = group_sum(hidden, down_weight, N_TP)
    return (middle.astype(jnp.float32) + lowered).astype(jnp.bfloat16)
```

```python
import functools

import jax
import jax.numpy as jnp
from jax import lax
from jax.experimental import pallas as pl
from jax.experimental.pallas import tpu as pltpu
from jax.sharding import PartitionSpec as P

REACH = 4


EPSILON = 1e-06
NEGATIVE = -1e30


def from_behind(value, axis, steps):
    count = lax.axis_size(axis)
    first, last = (max(0, -steps), min(count, count - steps))
    return lax.ppermute(value, axis, [(source, source + steps) for source in range(first, last)])


def normalize(middle, gain):
    widened = middle.astype(jnp.float32)
    factor = lax.rsqrt(jnp.mean(widened * widened, axis=-1, keepdims=True) + EPSILON)
    return (widened * factor * gain).astype(jnp.bfloat16)


def plain_local(
    residual,
    queries,
    keys,
    values,
    gate_cache,
    doc_ids,
    out_weight,
    mix_gain,
    gate_weight,
    up_weight,
    down_weight,
):
    tok_rows = queries.shape[0]
    heads_here = gate_cache.shape[1]
    head_size = queries.shape[1] // heads_here
    sp_index = lax.axis_index("sp")
    key_parts = [keys]
    value_parts = [values]
    cache_parts = [gate_cache]
    doc_parts = [doc_ids]
    for distance in range(1, REACH + 1):
        moved_keys, moved_values = from_behind((keys, values), "sp", distance)
        moved_cache, moved_docs = from_behind((gate_cache, doc_ids), "sp", distance)
        key_parts.append(moved_keys)
        value_parts.append(moved_values)
        cache_parts.append(moved_cache)
        doc_parts.append(moved_docs)
    all_keys = jnp.concatenate(key_parts[::-1], axis=0)
    all_values = jnp.concatenate(value_parts[::-1], axis=0)
    all_cache = jnp.concatenate(cache_parts[::-1], axis=0)
    all_docs = jnp.concatenate(doc_parts[::-1], axis=0)
    key_count = all_keys.shape[0]
    query_pos = sp_index * tok_rows + jnp.arange(tok_rows, dtype=jnp.int32)
    key_pos = (sp_index - REACH) * tok_rows + jnp.arange(key_count, dtype=jnp.int32)
    visible = (
        (key_pos[None, :] <= query_pos[:, None])
        & (key_pos[None, :] >= 0)
        & (all_docs[None, :] == doc_ids[:, None])
    )
    query_heads = queries.reshape(tok_rows, heads_here, head_size)
    key_heads = all_keys.reshape(key_count, heads_here, head_size)
    value_heads = all_values.reshape(key_count, heads_here, head_size)
    score_scale = head_size ** (-0.5)
    scores = (
        jnp.einsum("qhd,khd->hqk", query_heads, key_heads, preferred_element_type=jnp.float32)
        * score_scale
    )
    scores = scores + gate_cache.T[:, :, None] - all_cache.T[:, None, :]
    scores = jnp.where(visible[None], scores, NEGATIVE)
    row_max = jnp.max(scores, axis=-1, keepdims=True)
    exp_scores = jnp.exp(scores - row_max)
    weights = (exp_scores / jnp.sum(exp_scores, axis=-1, keepdims=True)).astype(jnp.bfloat16)
    attended = jnp.einsum("hqk,khd->qhd", weights, value_heads, preferred_element_type=jnp.float32)
    attended = attended.astype(jnp.bfloat16).reshape(tok_rows, heads_here * head_size)
    row_share = tok_rows // lax.axis_size("tp")
    tp_index = lax.axis_index("tp")
    partial_value = jnp.dot(attended, out_weight, preferred_element_type=jnp.float32)
    attn_sum = lax.psum(partial_value.astype(jnp.bfloat16), "tp").astype(jnp.float32)
    whole_middle = (residual.astype(jnp.float32) + attn_sum).astype(jnp.bfloat16)
    mixer_in = normalize(whole_middle, mix_gain)
    middle = lax.dynamic_slice_in_dim(whole_middle, tp_index * row_share, row_share, 0)
    held_gate, held_up = (
        lax.all_gather(gate_weight, "sp", axis=0, tiled=True),
        lax.all_gather(up_weight, "sp", axis=0, tiled=True),
    )
    gate_proj = jnp.dot(mixer_in, held_gate, preferred_element_type=jnp.float32)
    up_proj = jnp.dot(mixer_in, held_up, preferred_element_type=jnp.float32)
    hidden = (jax.nn.silu(gate_proj) * up_proj).astype(jnp.bfloat16)
    partials = jnp.dot(
        hidden,
        lax.all_gather(down_weight, "sp", axis=1, tiled=True),
        preferred_element_type=jnp.float32,
    )
    down_sum = lax.psum_scatter(
        partials.astype(jnp.bfloat16), "tp", scatter_dimension=0, tiled=True
    ).astype(jnp.float32)
    return (middle.astype(jnp.float32) + down_sum).astype(jnp.bfloat16)


ROWS = 128


def attend_tile(tile, plane_index, span, head_size, queries, keys, values, aux, out):
    heads = queries.shape[1] // head_size
    q_start = pl.multiple_of(tile * ROWS, ROWS)
    window = span + ROWS
    key_aux = aux[:, pl.ds(q_start, window)]
    query_aux = jnp.transpose(aux[:, pl.ds(pl.multiple_of(q_start + span, ROWS), ROWS)])
    column = lax.broadcasted_iota(jnp.int32, (ROWS, window), 1)
    row = lax.broadcasted_iota(jnp.int32, (ROWS, window), 0)
    first = (1 - plane_index) * span - q_start
    visible = (
        (column <= row + span)
        & (column >= first)
        & (key_aux[heads : heads + 1, :] == query_aux[:, heads : heads + 1])
    )
    query = queries[pl.ds(q_start, ROWS), :] * jnp.bfloat16(head_size ** (-0.5))
    parts = []
    for head in range(heads):
        lanes = slice(head * head_size, (head + 1) * head_size)
        key = keys[pl.ds(q_start, window), lanes]
        scores = lax.dot_general(
            query[:, lanes], key, (((1,), (1,)), ((), ())), preferred_element_type=jnp.float32
        )
        scores = scores + (query_aux[:, head : head + 1] - key_aux[head : head + 1, :])
        scores = jnp.where(visible, scores, NEGATIVE)
        exp_scores = jnp.exp(scores - jnp.max(scores, axis=-1, keepdims=True))
        total = jnp.sum(exp_scores, axis=-1, keepdims=True)
        mixed = jnp.dot(
            exp_scores.astype(jnp.bfloat16),
            values[pl.ds(q_start, window), lanes],
            preferred_element_type=jnp.float32,
        )
        parts.append(mixed / total)
    out[pl.ds(q_start, ROWS), :] = jnp.concatenate(parts, axis=1).astype(jnp.bfloat16)


def attend_kernel(
    planes, group, head_size,
    queries, keys, values, aux, gate, up, down,
    attended, gate_all, up_all, down_all,
    q_buf, k_buf, v_buf, aux_buf, out_buf,
    a_send, a_recv, a_own, h_send, h_recv, w_send, w_recv, g_send, g_recv, w_own, b_send, b_recv, b_own,
):
    me = lax.axis_index("sp")
    plane, place = me // group, lax.rem(me, group)
    tok = queries.shape[0]
    cols = queries.shape[1] // group
    span = tok * group
    depth = gate.shape[0]
    width = gate.shape[1] // planes
    MESH = pl.DeviceIdType.MESH

    def neighbour(step):
        return lax.rem(place + step, group)

    def in_plane(step):
        return {"sp": plane * group + neighbour(step)}

    def other_plane(step):
        return lax.rem(plane + step, planes)

    def across(step):
        return {"sp": other_plane(step) * group + place}

    barrier = pltpu.get_barrier_semaphore()
    for step in range(1, group):
        pl.semaphore_signal(barrier, inc=1, device_id=in_plane(step), device_id_type=MESH)
    for step in range(1, planes):
        pl.semaphore_signal(barrier, inc=1, device_id=across(step), device_id_type=MESH)
    pl.semaphore_wait(barrier, group + planes - 2)

    def remote(src, dst, send, recv, device):
        return pltpu.make_async_remote_copy(
            src_ref=src, dst_ref=dst, send_sem=send, recv_sem=recv,
            device_id=device, device_id_type=MESH,
        )

    own_rows = pl.ds(pl.multiple_of(span + place * tok, 128), tok)
    q_rows = pl.ds(pl.multiple_of(place * tok, 128), tok)

    def head_cols(index):
        return pl.ds(pl.multiple_of(index * cols, 128), cols)

    spread = []
    for step in range(1, group):
        to = neighbour(step)
        for i, (src, dst, rows) in enumerate(
            ((keys, k_buf, own_rows), (values, v_buf, own_rows), (queries, q_buf, q_rows))
        ):
            spread.append(remote(src.at[:, head_cols(to)], dst.at[rows, :],
                                 a_send.at[i, step], a_recv.at[i, step], in_plane(step)))
        spread.append(remote(aux.at[to], aux_buf.at[:, own_rows],
                             a_send.at[3, step], a_recv.at[3, step], in_plane(step)))
    own = [
        pltpu.make_async_copy(keys.at[:, head_cols(place)], k_buf.at[own_rows, :], a_own.at[0]),
        pltpu.make_async_copy(values.at[:, head_cols(place)], v_buf.at[own_rows, :], a_own.at[1]),
        pltpu.make_async_copy(queries.at[:, head_cols(place)], q_buf.at[q_rows, :], a_own.at[2]),
        pltpu.make_async_copy(aux.at[place], aux_buf.at[:, own_rows], a_own.at[3]),
    ]
    for copy in spread + own:
        copy.start()

    def piece(m, part):
        at = pl.ds(pl.multiple_of(part * width, 128), width)
        return down.at[at, :] if m == 2 else (gate, up)[m].at[:, at]

    def slot(m, source_plane):
        at = pl.ds(pl.multiple_of((source_plane * group + place) * depth, 128), depth)
        return down_all.at[:, at] if m == 2 else (gate_all, up_all)[m].at[at, :]

    first = {
        (m, step): remote(piece(m, other_plane(step)), slot(m, plane),
                          w_send.at[m, step], w_recv.at[m, step], across(step))
        for m in range(3) for step in range(1, planes)
    }
    second = {}
    kept = [pltpu.make_async_copy(piece(m, plane), slot(m, plane), w_own.at[m]) for m in range(3)]
    for copy in kept:
        copy.start()

    def forward(m, source_step):
        source = lax.rem(plane + planes - source_step, planes)
        for step in range(1, group):
            src = piece(m, plane) if source_step == 0 else slot(m, source)
            copy = remote(src, slot(m, source), g_send.at[m, source_step, step],
                          g_recv.at[m, source_step, step], in_plane(step))
            copy.start()
            second[m, source_step, step] = copy

    for step in range(1, planes):
        first[0, step].start()
    for copy in own:
        copy.wait()
    for copy in spread:
        copy.wait()
    late, early = pl.ds(span, span), pl.ds(0, span)
    halo = [
        remote(k_buf.at[late, :], k_buf.at[early, :], h_send.at[0], h_recv.at[0], across(1)),
        remote(v_buf.at[late, :], v_buf.at[early, :], h_send.at[1], h_recv.at[1], across(1)),
        remote(aux_buf.at[:, late], aux_buf.at[:, early], h_send.at[2], h_recv.at[2], across(1)),
    ]
    for copy in halo:
        copy.start()
    for m in range(1, 3):
        for step in range(1, planes):
            first[m, step].start()
    for m in range(3):
        forward(m, 0)
    for m in range(3):
        for step in range(1, planes):
            first[m, step].wait()
            forward(m, step)
    for copy in halo:
        copy.wait()

    def one(tile, carry):
        attend_tile(tile, plane, span, head_size, q_buf, k_buf, v_buf, aux_buf, out_buf)
        return carry

    lax.fori_loop(0, span // ROWS, one, 0)

    back = []
    for step in range(1, group):
        rows = pl.ds(pl.multiple_of(neighbour(step) * tok, 128), tok)
        back.append(remote(out_buf.at[rows, :], attended.at[:, head_cols(place)],
                           b_send.at[step], b_recv.at[step], in_plane(step)))
    stay = pltpu.make_async_copy(out_buf.at[q_rows, :], attended.at[:, head_cols(place)], b_own)
    for copy in back:
        copy.start()
    stay.start()
    stay.wait()
    for copy in back + kept:
        copy.wait()
    for copy in second.values():
        copy.wait()


def attend_and_gather(queries, keys, values, aux, gate, up, down, planes, group, head_size):
    tok, all_cols = queries.shape
    cols, span = all_cols // group, tok * group
    features, width = gate.shape[0] * planes * group, gate.shape[1] // planes
    sem = pltpu.SemaphoreType.DMA
    anywhere = pl.BlockSpec(memory_space=pl.ANY)
    bf16 = jnp.bfloat16
    return pl.pallas_call(
        functools.partial(attend_kernel, planes, group, head_size),
        out_shape=(
            jax.ShapeDtypeStruct((tok, all_cols), bf16),
            jax.ShapeDtypeStruct((features, width), bf16),
            jax.ShapeDtypeStruct((features, width), bf16),
            jax.ShapeDtypeStruct((width, features), bf16),
        ),
        in_specs=[anywhere] * 7,
        out_specs=(anywhere,) * 4,
        scratch_shapes=[
            pltpu.VMEM((span, cols), bf16),
            pltpu.VMEM((2 * span, cols), bf16),
            pltpu.VMEM((2 * span, cols), bf16),
            pltpu.VMEM((8, 2 * span), jnp.float32),
            pltpu.VMEM((span, cols), bf16),
            sem((4, group)), sem((4, group)), sem((4,)),
            sem((3,)), sem((3,)),
            sem((3, planes)), sem((3, planes)),
            sem((3, planes, group)), sem((3, planes, group)),
            sem((3,)),
            sem((group,)), sem((group,)), sem,
        ],
        compiler_params=pltpu.CompilerParams(
            collective_id=0, has_side_effects=True, vmem_limit_bytes=40 * 1024 * 1024
        ),
    )(queries, keys, values, aux, gate, up, down)


def grouped_local(
    planes, group,
    residual, queries, keys, values, gate_cache, doc_ids,
    out_weight, mix_gain, gate_weight, up_weight, down_weight,
):
    tok_rows = queries.shape[0]
    heads_here = gate_cache.shape[1]
    head_size = queries.shape[1] // heads_here
    heads = heads_here // group
    rows = gate_cache.T.reshape(group, heads, tok_rows)
    docs = jnp.broadcast_to(doc_ids.astype(jnp.float32), (group, 1, tok_rows))
    fill = jnp.zeros((group, 7 - heads, tok_rows), jnp.float32)
    aux = jnp.concatenate([rows, docs, fill], axis=1)
    attended, gate, up, down = attend_and_gather(
        queries, keys, values, aux, gate_weight, up_weight, down_weight, planes, group, head_size
    )
    tp_count = lax.axis_size("tp")
    row_share = tok_rows // tp_count
    tp_index = lax.axis_index("tp")
    partial_value = jnp.dot(attended, out_weight, preferred_element_type=jnp.float32)
    return finish(
        planes, group, residual, partial_value.astype(jnp.bfloat16), mix_gain, gate, up, down,
        row_share, tp_index,
    )


def finish(planes, group, residual, partial_value, mix_gain, gate, up, down, row_share, tp_index):
    peers = [[plane * group + place for plane in range(planes)] for place in range(group)]
    attn_sum = lax.psum(partial_value, "tp").astype(jnp.float32)
    whole_middle = (residual.astype(jnp.float32) + attn_sum).astype(jnp.bfloat16)
    mixer_in = normalize(whole_middle, mix_gain)
    middle = lax.dynamic_slice_in_dim(whole_middle, tp_index * row_share, row_share, 0)
    tokens = lax.all_gather(mixer_in, "sp", axis=0, tiled=True, axis_index_groups=peers)
    gate_proj = jnp.dot(tokens, gate, preferred_element_type=jnp.float32)
    up_proj = jnp.dot(tokens, up, preferred_element_type=jnp.float32)
    hidden = (jax.nn.silu(gate_proj) * up_proj).astype(jnp.bfloat16)
    partials = jnp.dot(hidden, down, preferred_element_type=jnp.float32).astype(jnp.bfloat16)
    mine = lax.psum_scatter(
        partials, "sp", scatter_dimension=0, tiled=True, axis_index_groups=peers
    )
    down_sum = lax.psum_scatter(mine, "tp", scatter_dimension=0, tiled=True).astype(jnp.float32)
    return (middle.astype(jnp.float32) + down_sum).astype(jnp.bfloat16)


def choose(
    residual, queries, keys, values, gate_cache, doc_ids,
    out_weight, mix_gain, gate_weight, up_weight, down_weight,
):
    arrays = (
        residual, queries, keys, values, gate_cache, doc_ids,
        out_weight, mix_gain, gate_weight, up_weight, down_weight,
    )
    count, group = lax.axis_size("sp"), REACH
    planes = count // group
    heads = gate_cache.shape[1] // group
    fits = (
        count == planes * group
        and gate_cache.shape[1] == heads * group
        and 1 <= heads <= 7
        and queries.shape[0] % 128 == 0
        and (queries.shape[1] // group) % 128 == 0
        and gate_weight.shape[0] % 128 == 0
        and gate_weight.shape[1] % (planes * 128) == 0
    )
    return grouped_local(planes, group, *arrays) if fits else plain_local(*arrays)


def solution(mesh):
    return jax.shard_map(
        choose,
        mesh=mesh,
        in_specs=(
            P("sp", None),
            P("sp", "tp"),
            P("sp", "tp"),
            P("sp", "tp"),
            P("sp", "tp"),
            P("sp"),
            P("tp", None),
            P(),
            P("sp", "tp"),
            P("sp", "tp"),
            P("tp", "sp"),
        ),
        out_specs=P(("sp", "tp"), None),
        check_vma=False,
    )
```

```python
import functools

import jax
import jax.numpy as jnp
from jax import lax
from jax.experimental import pallas as pl
from jax.experimental.pallas import tpu as pltpu
from jax.sharding import PartitionSpec as P

REACH = 4


EPSILON = 1e-06
NEGATIVE = -1e30


def from_behind(value, axis, steps):
    count = lax.axis_size(axis)
    first, last = (max(0, -steps), min(count, count - steps))
    return lax.ppermute(value, axis, [(source, source + steps) for source in range(first, last)])


def normalize(middle, gain):
    widened = middle.astype(jnp.float32)
    factor = lax.rsqrt(jnp.mean(widened * widened, axis=-1, keepdims=True) + EPSILON)
    return (widened * factor * gain).astype(jnp.bfloat16)


def plain_local(
    residual,
    queries,
    keys,
    values,
    gate_cache,
    doc_ids,
    out_weight,
    mix_gain,
    gate_weight,
    up_weight,
    down_weight,
):
    tok_rows = queries.shape[0]
    heads_here = gate_cache.shape[1]
    head_size = queries.shape[1] // heads_here
    sp_index = lax.axis_index("sp")
    key_parts = [keys]
    value_parts = [values]
    cache_parts = [gate_cache]
    doc_parts = [doc_ids]
    for distance in range(1, REACH + 1):
        moved_keys, moved_values = from_behind((keys, values), "sp", distance)
        moved_cache, moved_docs = from_behind((gate_cache, doc_ids), "sp", distance)
        key_parts.append(moved_keys)
        value_parts.append(moved_values)
        cache_parts.append(moved_cache)
        doc_parts.append(moved_docs)
    all_keys = jnp.concatenate(key_parts[::-1], axis=0)
    all_values = jnp.concatenate(value_parts[::-1], axis=0)
    all_cache = jnp.concatenate(cache_parts[::-1], axis=0)
    all_docs = jnp.concatenate(doc_parts[::-1], axis=0)
    key_count = all_keys.shape[0]
    query_pos = sp_index * tok_rows + jnp.arange(tok_rows, dtype=jnp.int32)
    key_pos = (sp_index - REACH) * tok_rows + jnp.arange(key_count, dtype=jnp.int32)
    visible = (
        (key_pos[None, :] <= query_pos[:, None])
        & (key_pos[None, :] >= 0)
        & (all_docs[None, :] == doc_ids[:, None])
    )
    query_heads = queries.reshape(tok_rows, heads_here, head_size)
    key_heads = all_keys.reshape(key_count, heads_here, head_size)
    value_heads = all_values.reshape(key_count, heads_here, head_size)
    score_scale = head_size ** (-0.5)
    scores = (
        jnp.einsum("qhd,khd->hqk", query_heads, key_heads, preferred_element_type=jnp.float32)
        * score_scale
    )
    scores = scores + gate_cache.T[:, :, None] - all_cache.T[:, None, :]
    scores = jnp.where(visible[None], scores, NEGATIVE)
    row_max = jnp.max(scores, axis=-1, keepdims=True)
    exp_scores = jnp.exp(scores - row_max)
    weights = (exp_scores / jnp.sum(exp_scores, axis=-1, keepdims=True)).astype(jnp.bfloat16)
    attended = jnp.einsum("hqk,khd->qhd", weights, value_heads, preferred_element_type=jnp.float32)
    attended = attended.astype(jnp.bfloat16).reshape(tok_rows, heads_here * head_size)
    row_share = tok_rows // lax.axis_size("tp")
    tp_index = lax.axis_index("tp")
    partial_value = jnp.dot(attended, out_weight, preferred_element_type=jnp.float32)
    attn_sum = lax.psum(partial_value.astype(jnp.bfloat16), "tp").astype(jnp.float32)
    whole_middle = (residual.astype(jnp.float32) + attn_sum).astype(jnp.bfloat16)
    mixer_in = normalize(whole_middle, mix_gain)
    middle = lax.dynamic_slice_in_dim(whole_middle, tp_index * row_share, row_share, 0)
    held_gate, held_up = (
        lax.all_gather(gate_weight, "sp", axis=0, tiled=True),
        lax.all_gather(up_weight, "sp", axis=0, tiled=True),
    )
    gate_proj = jnp.dot(mixer_in, held_gate, preferred_element_type=jnp.float32)
    up_proj = jnp.dot(mixer_in, held_up, preferred_element_type=jnp.float32)
    hidden = (jax.nn.silu(gate_proj) * up_proj).astype(jnp.bfloat16)
    partials = jnp.dot(
        hidden,
        lax.all_gather(down_weight, "sp", axis=1, tiled=True),
        preferred_element_type=jnp.float32,
    )
    down_sum = lax.psum_scatter(
        partials.astype(jnp.bfloat16), "tp", scatter_dimension=0, tiled=True
    ).astype(jnp.float32)
    return (middle.astype(jnp.float32) + down_sum).astype(jnp.bfloat16)


ROWS = 128


def attend_tile(tile, plane_index, span, head_size, queries, keys, values, aux, out):
    heads = queries.shape[1] // head_size
    q_start = pl.multiple_of(tile * ROWS, ROWS)
    window = span + ROWS
    key_aux = aux[:, pl.ds(q_start, window)]
    query_aux = jnp.transpose(aux[:, pl.ds(pl.multiple_of(q_start + span, ROWS), ROWS)])
    column = lax.broadcasted_iota(jnp.int32, (ROWS, window), 1)
    row = lax.broadcasted_iota(jnp.int32, (ROWS, window), 0)
    first = (1 - plane_index) * span - q_start
    visible = (
        (column <= row + span)
        & (column >= first)
        & (key_aux[heads : heads + 1, :] == query_aux[:, heads : heads + 1])
    )
    query = queries[pl.ds(q_start, ROWS), :] * jnp.bfloat16(head_size ** (-0.5))
    parts = []
    for head in range(heads):
        lanes = slice(head * head_size, (head + 1) * head_size)
        key = keys[pl.ds(q_start, window), lanes]
        scores = lax.dot_general(
            query[:, lanes], key, (((1,), (1,)), ((), ())), preferred_element_type=jnp.float32
        )
        scores = scores + (query_aux[:, head : head + 1] - key_aux[head : head + 1, :])
        scores = jnp.where(visible, scores, NEGATIVE)
        exp_scores = jnp.exp(scores - jnp.max(scores, axis=-1, keepdims=True))
        total = jnp.sum(exp_scores, axis=-1, keepdims=True)
        mixed = jnp.dot(
            exp_scores.astype(jnp.bfloat16),
            values[pl.ds(q_start, window), lanes],
            preferred_element_type=jnp.float32,
        )
        parts.append(mixed / total)
    out[pl.ds(q_start, ROWS), :] = jnp.concatenate(parts, axis=1).astype(jnp.bfloat16)


def attend_kernel(
    planes, group, head_size,
    queries, keys, values, aux, gate, up, down,
    attended, gate_all, up_all, down_all,
    q_buf, k_buf, v_buf, aux_buf, out_buf,
    a_send, a_recv, a_own, h_send, h_recv, w_send, w_recv, g_send, g_recv, w_own, b_send, b_recv, b_own,
):
    me = lax.axis_index("sp")
    plane, place = me // group, lax.rem(me, group)
    tok = queries.shape[0]
    cols = queries.shape[1] // group
    span = tok * group
    depth = gate.shape[0]
    width = gate.shape[1] // planes
    MESH = pl.DeviceIdType.MESH

    def neighbour(step):
        return lax.rem(place + step, group)

    def in_plane(step):
        return {"sp": plane * group + neighbour(step)}

    def other_plane(step):
        return lax.rem(plane + step, planes)

    def across(step):
        return {"sp": other_plane(step) * group + place}

    barrier = pltpu.get_barrier_semaphore()
    for step in range(1, group):
        pl.semaphore_signal(barrier, inc=1, device_id=in_plane(step), device_id_type=MESH)
    for step in range(1, planes):
        pl.semaphore_signal(barrier, inc=1, device_id=across(step), device_id_type=MESH)
    pl.semaphore_wait(barrier, group + planes - 2)

    def remote(src, dst, send, recv, device):
        return pltpu.make_async_remote_copy(
            src_ref=src, dst_ref=dst, send_sem=send, recv_sem=recv,
            device_id=device, device_id_type=MESH,
        )

    own_rows = pl.ds(pl.multiple_of(span + place * tok, 128), tok)
    q_rows = pl.ds(pl.multiple_of(place * tok, 128), tok)

    def head_cols(index):
        return pl.ds(pl.multiple_of(index * cols, 128), cols)

    spread = []
    for step in range(1, group):
        to = neighbour(step)
        for i, (src, dst, rows) in enumerate(
            ((keys, k_buf, own_rows), (values, v_buf, own_rows), (queries, q_buf, q_rows))
        ):
            spread.append(remote(src.at[:, head_cols(to)], dst.at[rows, :],
                                 a_send.at[i, step], a_recv.at[i, step], in_plane(step)))
        spread.append(remote(aux.at[to], aux_buf.at[:, own_rows],
                             a_send.at[3, step], a_recv.at[3, step], in_plane(step)))
    own = [
        pltpu.make_async_copy(keys.at[:, head_cols(place)], k_buf.at[own_rows, :], a_own.at[0]),
        pltpu.make_async_copy(values.at[:, head_cols(place)], v_buf.at[own_rows, :], a_own.at[1]),
        pltpu.make_async_copy(queries.at[:, head_cols(place)], q_buf.at[q_rows, :], a_own.at[2]),
        pltpu.make_async_copy(aux.at[place], aux_buf.at[:, own_rows], a_own.at[3]),
    ]
    for copy in spread + own:
        copy.start()

    def piece(m, part):
        at = pl.ds(pl.multiple_of(part * width, 128), width)
        return down.at[at, :] if m == 2 else (gate, up)[m].at[:, at]

    def slot(m, source_plane):
        at = pl.ds(pl.multiple_of((source_plane * group + place) * depth, 128), depth)
        return down_all.at[:, at] if m == 2 else (gate_all, up_all)[m].at[at, :]

    first = {
        (m, step): remote(piece(m, other_plane(step)), slot(m, plane),
                          w_send.at[m, step], w_recv.at[m, step], across(step))
        for m in range(3) for step in range(1, planes)
    }
    second = {}
    kept = [pltpu.make_async_copy(piece(m, plane), slot(m, plane), w_own.at[m]) for m in range(3)]
    for copy in kept:
        copy.start()

    def forward(m, source_step):
        source = lax.rem(plane + planes - source_step, planes)
        for step in range(1, group):
            src = piece(m, plane) if source_step == 0 else slot(m, source)
            copy = remote(src, slot(m, source), g_send.at[m, source_step, step],
                          g_recv.at[m, source_step, step], in_plane(step))
            copy.start()
            second[m, source_step, step] = copy

    for step in range(1, planes):
        first[0, step].start()
    for copy in own:
        copy.wait()
    for copy in spread:
        copy.wait()
    late, early = pl.ds(span, span), pl.ds(0, span)
    halo = [
        remote(k_buf.at[late, :], k_buf.at[early, :], h_send.at[0], h_recv.at[0], across(1)),
        remote(v_buf.at[late, :], v_buf.at[early, :], h_send.at[1], h_recv.at[1], across(1)),
        remote(aux_buf.at[:, late], aux_buf.at[:, early], h_send.at[2], h_recv.at[2], across(1)),
    ]
    for copy in halo:
        copy.start()
    for m in range(1, 3):
        for step in range(1, planes):
            first[m, step].start()
    for m in range(3):
        forward(m, 0)
    for m in range(3):
        for step in range(1, planes):
            first[m, step].wait()
            forward(m, step)
    for copy in halo:
        copy.wait()

    def one(tile, carry):
        attend_tile(tile, plane, span, head_size, q_buf, k_buf, v_buf, aux_buf, out_buf)
        return carry

    lax.fori_loop(0, span // ROWS, one, 0)

    back = []
    for step in range(1, group):
        rows = pl.ds(pl.multiple_of(neighbour(step) * tok, 128), tok)
        back.append(remote(out_buf.at[rows, :], attended.at[:, head_cols(place)],
                           b_send.at[step], b_recv.at[step], in_plane(step)))
    stay = pltpu.make_async_copy(out_buf.at[q_rows, :], attended.at[:, head_cols(place)], b_own)
    for copy in back:
        copy.start()
    stay.start()
    stay.wait()
    for copy in back + kept:
        copy.wait()
    for copy in second.values():
        copy.wait()


def attend_and_gather(queries, keys, values, aux, gate, up, down, planes, group, head_size):
    tok, all_cols = queries.shape
    cols, span = all_cols // group, tok * group
    features, width = gate.shape[0] * planes * group, gate.shape[1] // planes
    sem = pltpu.SemaphoreType.DMA
    anywhere = pl.BlockSpec(memory_space=pl.ANY)
    bf16 = jnp.bfloat16
    return pl.pallas_call(
        functools.partial(attend_kernel, planes, group, head_size),
        out_shape=(
            jax.ShapeDtypeStruct((tok, all_cols), bf16),
            jax.ShapeDtypeStruct((features, width), bf16),
            jax.ShapeDtypeStruct((features, width), bf16),
            jax.ShapeDtypeStruct((width, features), bf16),
        ),
        in_specs=[anywhere] * 7,
        out_specs=(anywhere,) * 4,
        scratch_shapes=[
            pltpu.VMEM((span, cols), bf16),
            pltpu.VMEM((2 * span, cols), bf16),
            pltpu.VMEM((2 * span, cols), bf16),
            pltpu.VMEM((8, 2 * span), jnp.float32),
            pltpu.VMEM((span, cols), bf16),
            sem((4, group)), sem((4, group)), sem((4,)),
            sem((3,)), sem((3,)),
            sem((3, planes)), sem((3, planes)),
            sem((3, planes, group)), sem((3, planes, group)),
            sem((3,)),
            sem((group,)), sem((group,)), sem,
        ],
        compiler_params=pltpu.CompilerParams(
            collective_id=0, has_side_effects=True, vmem_limit_bytes=40 * 1024 * 1024
        ),
    )(queries, keys, values, aux, gate, up, down)


def grouped_local(
    planes, group,
    residual, queries, keys, values, gate_cache, doc_ids,
    out_weight, mix_gain, gate_weight, up_weight, down_weight,
):
    tok_rows = queries.shape[0]
    heads_here = gate_cache.shape[1]
    head_size = queries.shape[1] // heads_here
    heads = heads_here // group
    rows = gate_cache.T.reshape(group, heads, tok_rows)
    docs = jnp.broadcast_to(doc_ids.astype(jnp.float32), (group, 1, tok_rows))
    fill = jnp.zeros((group, 7 - heads, tok_rows), jnp.float32)
    aux = jnp.concatenate([rows, docs, fill], axis=1)
    attended, gate, up, down = attend_and_gather(
        queries, keys, values, aux, gate_weight, up_weight, down_weight, planes, group, head_size
    )
    tp_count = lax.axis_size("tp")
    row_share = tok_rows // tp_count
    tp_index = lax.axis_index("tp")
    partial_value = jnp.dot(attended, out_weight, preferred_element_type=jnp.float32)
    return finish(
        planes, group, residual, partial_value.astype(jnp.bfloat16), mix_gain, gate, up, down,
        row_share, tp_index,
    )


def mix_kernel(
    planes, group,
    partial, residual, gain, gate, up, down, out,
    got, tokens, part, pair, sums, inbox, mid,
    x_send, x_recv, n_send, n_recv, z_send, z_recv, p_send, p_recv, r_send, r_recv,
):
    me, core = lax.axis_index("sp"), lax.axis_index("tp")
    plane, place = me // group, lax.rem(me, group)
    half, features = mid.shape
    other = 1 - core
    partner = {"tp": other}
    MESH = pl.DeviceIdType.MESH

    def across(step):
        return {"sp": lax.rem(plane + step, planes) * group + place}

    barrier = pltpu.get_barrier_semaphore()
    pl.semaphore_signal(barrier, inc=1, device_id=partner, device_id_type=MESH)
    for step in range(1, planes):
        pl.semaphore_signal(barrier, inc=1, device_id=across(step), device_id_type=MESH)
    pl.semaphore_wait(barrier, planes)

    def remote(src, dst, send, recv, device):
        copy = pltpu.make_async_remote_copy(
            src_ref=src, dst_ref=dst, send_sem=send, recv_sem=recv,
            device_id=device, device_id_type=MESH,
        )
        copy.start()
        return copy

    theirs = pl.ds(pl.multiple_of(other * half, 32), half)
    remote(partial.at[theirs, :], got, x_send, x_recv, partner).wait()
    chunk = 32

    def middle_rows(i, carry):
        at = pl.ds(pl.multiple_of(i * chunk, chunk), chunk)
        full = pl.ds(pl.multiple_of(core * half + i * chunk, chunk), chunk)
        total = partial[full, :].astype(jnp.float32) + got[at, :].astype(jnp.float32)
        middle = (residual[full, :].astype(jnp.float32) + total).astype(jnp.bfloat16)
        mid[at, :] = middle
        tokens[plane, core, at, :] = normalize(middle, gain[...])
        return carry

    lax.fori_loop(0, half // chunk, middle_rows, 0)
    mine = tokens.at[plane, core]
    near = [remote(mine, mine, n_send.at[0], n_recv.at[0], partner)]
    far = [None] + [
        remote(mine, mine, z_send.at[e], z_recv.at[e], across(e)) for e in range(1, planes)
    ]
    pairs, back = [], [None]
    for e in range(planes):
        source = lax.rem(plane + planes - e, planes)
        if e > 0:
            far[e].wait_recv()
            held = tokens.at[source, core]
            near.append(remote(held, held, n_send.at[e], n_recv.at[e], partner))
        near[e].wait_recv()
        block = tokens[source].reshape(2 * half, features)
        gate_proj = jnp.dot(block, gate[...], preferred_element_type=jnp.float32)
        up_proj = jnp.dot(block, up[...], preferred_element_type=jnp.float32)
        hidden = (gate_proj / (1.0 + jnp.exp(-gate_proj)) * up_proj).astype(jnp.bfloat16)
        lowered = jnp.dot(hidden, down[...], preferred_element_type=jnp.float32)
        part[source] = lowered.astype(jnp.bfloat16).reshape(2, half, features)
        pairs.append(remote(part.at[source, other], pair.at[source],
                            p_send.at[e], p_recv.at[e], partner))
        if e > 0:
            pairs[e].wait_recv()
            both = part[source, core].astype(jnp.float32) + pair[source].astype(jnp.float32)
            sums[source] = both.astype(jnp.bfloat16)
            back.append(remote(sums.at[source], inbox.at[e],
                               r_send.at[e], r_recv.at[e], across(planes - e)))
    pairs[0].wait_recv()
    for e in range(1, planes):
        back[e].wait_recv()

    def last_rows(i, carry):
        at = pl.ds(pl.multiple_of(i * chunk, chunk), chunk)
        total = part[plane, core, at, :].astype(jnp.float32)
        total = total + pair[plane, at, :].astype(jnp.float32)
        for e in range(1, planes):
            total = total + inbox[e, at, :].astype(jnp.float32)
        out[at, :] = (mid[at, :].astype(jnp.float32) + total).astype(jnp.bfloat16)
        return carry

    lax.fori_loop(0, half // chunk, last_rows, 0)
    for copy in near + far[1:] + pairs + back[1:]:
        copy.wait_send()


def finish(planes, group, residual, partial_value, mix_gain, gate, up, down, row_share, tp_index):
    features = residual.shape[1]
    sem = pltpu.SemaphoreType.DMA
    local_spec = pl.BlockSpec(memory_space=pltpu.VMEM)
    bf16 = jnp.bfloat16
    several = sem((planes,))
    return pl.pallas_call(
        functools.partial(mix_kernel, planes, group),
        out_shape=jax.ShapeDtypeStruct((row_share, features), bf16),
        in_specs=[local_spec] * 6,
        out_specs=local_spec,
        scratch_shapes=[
            pltpu.VMEM((row_share, features), bf16),
            pltpu.VMEM((planes, 2, row_share, features), bf16),
            pltpu.VMEM((planes, 2, row_share, features), bf16),
            pltpu.VMEM((planes, row_share, features), bf16),
            pltpu.VMEM((planes, row_share, features), bf16),
            pltpu.VMEM((planes, row_share, features), bf16),
            pltpu.VMEM((row_share, features), bf16),
            sem, sem, several, several, several, several, several, several, several, several,
        ],
        compiler_params=pltpu.CompilerParams(
            collective_id=1, has_side_effects=True, vmem_limit_bytes=58 * 1024 * 1024
        ),
    )(partial_value, residual, mix_gain.reshape(1, features), gate, up, down)


def choose(
    residual, queries, keys, values, gate_cache, doc_ids,
    out_weight, mix_gain, gate_weight, up_weight, down_weight,
):
    arrays = (
        residual, queries, keys, values, gate_cache, doc_ids,
        out_weight, mix_gain, gate_weight, up_weight, down_weight,
    )
    count, group = lax.axis_size("sp"), REACH
    planes = count // group
    heads = gate_cache.shape[1] // group
    fits = (
        count == planes * group
        and lax.axis_size("tp") == 2
        and queries.shape[0] % 64 == 0
        and gate_cache.shape[1] == heads * group
        and 1 <= heads <= 7
        and queries.shape[0] % 128 == 0
        and (queries.shape[1] // group) % 128 == 0
        and gate_weight.shape[0] % 128 == 0
        and gate_weight.shape[1] % (planes * 128) == 0
    )
    return grouped_local(planes, group, *arrays) if fits else plain_local(*arrays)


def solution(mesh):
    return jax.shard_map(
        choose,
        mesh=mesh,
        in_specs=(
            P("sp", None),
            P("sp", "tp"),
            P("sp", "tp"),
            P("sp", "tp"),
            P("sp", "tp"),
            P("sp"),
            P("tp", None),
            P(),
            P("sp", "tp"),
            P("sp", "tp"),
            P("tp", "sp"),
        ),
        out_specs=P(("sp", "tp"), None),
        check_vma=False,
    )
```
